128 devices in a mesh: rep: 2 (over z_hi), fs: 32 (over z_lo, y, x), tp: 2 (over core).
Axes of the slice: x: 4, y: 4, z: 4 (z_hi: 2, z_lo: 2; z = z_hi * 2 + z_lo), core: 2. Of those that a mesh axis runs over, the one named last changes fastest.
Arguments:
- tokens: bfloat16 [64, 1024, 2048], P(('rep', 'fs'), 'tp'), may hold values from -6 to 6
- mix_gain: float32 [2048], replicated, may hold values from 0.1 to 1.9
- out_gate_w: float32 [2048, 1024], P('fs', 'tp'), may hold values from -0.125 to 0.125
- in_gate_w: float32 [2048, 1024], P('fs', 'tp'), may hold values from -0.125 to 0.125
- value_w: float32 [2048, 1024], P('fs', 'tp'), may hold values from -0.125 to 0.125
- out_gate_scale: float32 [1024], P(('tp', 'fs')), may hold values from 0.28 to 3.5
- in_gate_scale: float32 [1024], P(('tp', 'fs')), may hold values from 0.5 to 2
- value_scale: float32 [1024], P(('tp', 'fs')), may hold values from 0.5 to 2
- mix_taps: float32 [3, 1024], P(None, 'tp'), may hold values from -3.5 to 3.5
- conv_gain: float32 [1024], P('tp'), may hold values from 0.1 to 1.9
- out_proj_w: float32 [1024, 2048], P('tp', 'fs'), may hold values from -0.1875 to 0.1875
- proj_scale: float32 [2048], P('fs'), may hold values from 0.5 to 2
- ffn_gain: float32 [2048], replicated, may hold values from 0.1 to 1.9
- gate_w: float32 [2048, 2816], P('fs', 'tp'), may hold values from -0.125 to 0.125
- up_w: float32 [2048, 2816], P('fs', 'tp'), may hold values from -0.125 to 0.125
- gate_scale: float32 [2816], P(('tp', 'fs')), may hold values from 0.5 to 2
- up_scale: float32 [2816], P(('tp', 'fs')), may hold values from 0.5 to 2
- gate_taps: float32 [3, 2816], P(None, 'tp'), may hold values from -3.5 to 3.5
- up_taps: float32 [3, 2816], P(None, 'tp'), may hold values from -3.5 to 3.5
- gate_bias: float32 [2816], P('tp'), may hold values from -3 to 3
- up_bias: float32 [2816], P('tp'), may hold values from -3 to 3
- down_w: float32 [2816, 2048], P('tp', 'fs'), may hold values from -0.109375 to 0.109375
- down_scale: float32 [2048], P('fs'), may hold values from 0.5 to 2
Outputs:
- layer_out: bfloat16 [64, 1024, 2048], P(('rep', 'fs'), 'tp')
The draws below stay inside these ranges and needn't reach their ends.
All inputs are finite; a program needn't handle non-finite values.
Results may differ from the reference program's by a relative error of at most 0.02.
Values may be sent and summed in bfloat16 or wider, within the bound.
No kernel may reach another device: no remote copies, remote signals or barrier semaphores. Data moves between devices by JAX's collectives and lax.ppermute only.
A program may use at most 128 MiB of HBM per device.

```python
import math
import jax
import jax.numpy as jnp
from jax import lax

D = 2048
CONV = 1024
FF = 2816
KW = 3
SEQ = 1024
SEQS = 64


def draw_out_gate_scale(key, part):
    ramp = jnp.exp(jnp.linspace(math.log(0.4), math.log(2.5), CONV)).astype(jnp.float32)
    noise = jax.random.uniform(key, (CONV,), jnp.float32, 0.7, 1.4)
    return ramp * noise


def block_scale(rng, dims, pieces, low, top_value):
    loudness, own = 1.0, jax.random.fold_in(rng, 6)
    for dim, blocks in pieces:
        steps = jnp.exp(jax.random.uniform(jax.random.fold_in(own, dim), (blocks,), jnp.float32, low / len(pieces), top_value / len(pieces)))
        loudness = loudness * jnp.repeat(steps, dims[dim] // blocks).reshape([-1 if axis == dim else 1 for axis in range(len(dims))])
    return loudness


def bell_draw(key, extent, width, limit, cuts=(), held_as=jnp.bfloat16):
    result = jax.random.normal(key, extent, jnp.float32) * width
    if len(cuts) > 0:
        result = block_scale(key, extent, cuts, -0.22, 0.18) * result
    return jnp.clip(result, min=-limit, max=limit).astype(held_as)


def setup_inputs(seed: int = 0) -> dict:
    streams_of = jax.random.split(jax.random.key(seed), 24)
    tokens = bell_draw(streams_of[0], (SEQS, SEQ, D), 1.0, 6.0, ((0, 64), (1, 2)))
    mix_gain = jnp.clip(1.0 + 0.18 * jax.random.normal(streams_of[1], (D,), jnp.float32), 0.1, 1.9)
    out_gate_w = bell_draw(streams_of[2], (D, CONV), D ** -0.5, 0.125, ((0, 32), (1, 2)), jnp.float32)
    in_gate_w = bell_draw(streams_of[3], (D, CONV), D ** -0.5, 0.125, ((0, 32), (1, 2)), jnp.float32)
    value_w = bell_draw(streams_of[4], (D, CONV), D ** -0.5, 0.125, ((0, 32), (1, 2)), jnp.float32)
    out_gate_scale = draw_out_gate_scale(jax.random.fold_in(streams_of[23], 71), 0)
    in_gate_scale = jnp.clip(jnp.exp(math.log(2.0) - 1.3862944 * jax.random.uniform(streams_of[6], (CONV,), jnp.float32) ** block_scale(streams_of[6], (CONV,), ((0, 64),), -0.2, 0.2)), 0.5, 2.0)
    value_scale = jnp.clip(jnp.exp(math.log(2.0) - 1.3862944 * jax.random.uniform(streams_of[7], (CONV,), jnp.float32) ** block_scale(streams_of[7], (CONV,), ((0, 64),), -0.2, 0.2)), 0.5, 2.0)
    mix_taps = bell_draw(streams_of[8], (KW, CONV), KW ** -0.5, 3.5, ((1, 2),), jnp.float32)
    conv_gain = jnp.clip(1.0 + 0.18 * jax.random.normal(streams_of[9], (CONV,), jnp.float32), 0.1, 1.9)
    out_proj_w = bell_draw(streams_of[10], (CONV, D), CONV ** -0.5, 0.1875, ((0, 2), (1, 32)), jnp.float32)
    proj_scale = jnp.clip(jnp.exp(math.log(2.0) - 1.3862944 * jax.random.uniform(streams_of[11], (D,), jnp.float32) ** block_scale(streams_of[11], (D,), ((0, 32),), -0.2, 0.2)), 0.5, 2.0)
    ffn_gain = jnp.clip(1.0 + 0.18 * jax.random.normal(streams_of[12], (D,), jnp.float32), 0.1, 1.9)
    gate_w = bell_draw(streams_of[13], (D, FF), D ** -0.5, 0.125, ((0, 32), (1, 2)), jnp.float32)
    up_w = bell_draw(streams_of[14], (D, FF), D ** -0.5, 0.125, ((0, 32), (1, 2)), jnp.float32)
    gate_scale = jnp.clip(jnp.exp(math.log(2.0) - 1.3862944 * jax.random.uniform(streams_of[15], (FF,), jnp.float32) ** block_scale(streams_of[15], (FF,), ((0, 64),), -0.2, 0.2)), 0.5, 2.0)
    up_scale = jnp.clip(jnp.exp(math.log(2.0) - 1.3862944 * jax.random.uniform(streams_of[16], (FF,), jnp.float32) ** block_scale(streams_of[16], (FF,), ((0, 64),), -0.2, 0.2)), 0.5, 2.0)
    gate_taps = bell_draw(streams_of[17], (KW, FF), KW ** -0.5, 3.5, ((1, 2),), jnp.float32)
    up_taps = bell_draw(streams_of[18], (KW, FF), KW ** -0.5, 3.5, ((1, 2),), jnp.float32)
    gate_bias = bell_draw(streams_of[19], (FF,), 0.5, 3.0, ((0, 2),), jnp.float32)
    up_bias = bell_draw(streams_of[20], (FF,), 0.5, 3.0, ((0, 2),), jnp.float32)
    down_w = bell_draw(streams_of[21], (FF, D), FF ** -0.5, 0.109375, ((0, 2), (1, 32)), jnp.float32)
    down_scale = jnp.clip(jnp.exp(math.log(2.0) - 1.3862944 * jax.random.uniform(streams_of[22], (D,), jnp.float32) ** block_scale(streams_of[22], (D,), ((0, 32),), -0.2, 0.2)), 0.5, 2.0)
    return {"tokens": tokens, "mix_gain": mix_gain, "out_gate_w": out_gate_w, "in_gate_w": in_gate_w, "value_w": value_w, "out_gate_scale": out_gate_scale, "in_gate_scale": in_gate_scale, "value_scale": value_scale, "mix_taps": mix_taps, "conv_gain": conv_gain, "out_proj_w": out_proj_w, "proj_scale": proj_scale, "ffn_gain": ffn_gain, "gate_w": gate_w, "up_w": up_w, "gate_scale": gate_scale, "up_scale": up_scale, "gate_taps": gate_taps, "up_taps": up_taps, "gate_bias": gate_bias, "up_bias": up_bias, "down_w": down_w, "down_scale": down_scale}


epsilon = 1e-06

def norm_rows(values, gain):
    return values * lax.rsqrt(lax.optimization_barrier(jnp.mean(values * values, axis=-1, keepdims=True)) + epsilon) * gain

def causal_taps(values, taps):
    kernel = taps.shape[0]
    length = values.shape[0]
    padded = jnp.pad(values, ((kernel - 1, 0), (0, 0)))
    total = jnp.zeros(values.shape, jnp.float32)
    for offset in range(kernel):
        total = total + taps[offset] * padded[offset:offset + length]
    return total

def reference(tokens, mix_gain, out_gate_w, in_gate_w, value_w, out_gate_scale, in_gate_scale, value_scale, mix_taps, conv_gain, out_proj_w, proj_scale, ffn_gain, gate_w, up_w, gate_scale, up_scale, gate_taps, up_taps, gate_bias, up_bias, down_w, down_scale):

    def project(left, weight, scale):
        return jnp.dot(left, weight.astype(jnp.bfloat16), preferred_element_type=jnp.float32) * scale

    def layer_one(sequence):
        resid = sequence.astype(jnp.float32)
        normed_in = norm_rows(resid, mix_gain).astype(jnp.bfloat16)
        out_gate = project(normed_in, out_gate_w, out_gate_scale).astype(jnp.bfloat16)
        in_gate = project(normed_in, in_gate_w, in_gate_scale).astype(jnp.bfloat16)
        value_in = project(normed_in, value_w, value_scale).astype(jnp.bfloat16)
        mixed_in = in_gate.astype(jnp.float32) * value_in.astype(jnp.float32)
        conv_out = (out_gate.astype(jnp.float32) * causal_taps(mixed_in, mix_taps)).astype(jnp.bfloat16)
        mixed = norm_rows(conv_out.astype(jnp.float32), conv_gain).astype(jnp.bfloat16)
        first = (resid + project(mixed, out_proj_w, proj_scale)).astype(jnp.bfloat16)
        resid_two = first.astype(jnp.float32)
        normed_ffn = norm_rows(resid_two, ffn_gain).astype(jnp.bfloat16)
        gate_pre = project(normed_ffn, gate_w, gate_scale).astype(jnp.bfloat16)
        up_pre = project(normed_ffn, up_w, up_scale).astype(jnp.bfloat16)
        gate_act = causal_taps(gate_pre.astype(jnp.float32), gate_taps) + gate_bias
        up_act = causal_taps(up_pre.astype(jnp.float32), up_taps) + up_bias
        hidden = (jax.nn.silu(gate_act) * up_act).astype(jnp.bfloat16)
        return (resid_two + project(hidden, down_w, down_scale)).astype(jnp.bfloat16)
    return lax.map(layer_one, tokens)
```

```python
import jax
import jax.numpy as jnp
from jax import lax
from jax.sharding import PartitionSpec as P


EPS = 1e-06
F32 = jnp.float32
BF16 = jnp.bfloat16
ALL = ("rep", "fs")
N = 4


def hop(value, dz=0, dy=0, dx=0):
    pairs = []
    for z in range(N):
        for y in range(N):
            for x in range(N):
                to = ((z + dz) % N) * 16 + ((y + dy) % N) * 4 + (x + dx) % N
                pairs.append((z * 16 + y * 4 + x, to))
    return lax.ppermute(value, ALL, pairs)


def swap(value):
    return lax.ppermute(value, "tp", [(0, 1), (1, 0)])


def placed(pieces, spots):
    out = jnp.zeros((len(pieces), *pieces[0].shape), pieces[0].dtype)
    for piece, spot in zip(pieces, spots):
        out = lax.dynamic_update_index_in_dim(out, piece, spot, 0)
    return out


def ring(value, axis, me, near):
    step = {axis: 1}
    back = {axis: -1}
    before = hop(value, **step)
    after = hop(value, **back)
    if near:
        far = hop(value, **{axis: 2})
    else:
        half = value.shape[0] // 2
        far = jnp.concatenate([hop(before[:half], **step), hop(after[half:], **back)], 0)
    return placed((value, before, after, far), (me, (me + 3) % 4, (me + 1) % 4, (me + 2) % 4))


def across(value):
    half = value.shape[0] // 2
    return jnp.concatenate([hop(value[:half], dz=1), hop(value[half:], dz=-1)], 0)


def zxy(value, at, flip):
    z, y, x = at
    wide = value.shape[1]
    both = placed((value, across(value)), (z, 1 - z))
    if flip:
        col = ring(both.reshape(-1, wide), "dy", y, False)
        full = ring(col.reshape(-1, wide), "dx", x, False)
        full = full.reshape(4, 4, 2, 64, wide).transpose(2, 1, 0, 3, 4)
    else:
        row = ring(both.reshape(-1, wide), "dx", x, False)
        full = ring(row.reshape(-1, wide), "dy", y, False)
        full = full.reshape(4, 4, 2, 64, wide).transpose(2, 0, 1, 3, 4)
    return full.reshape(-1, wide)


def xyz(value, at, flip):
    z, y, x = at
    wide = value.shape[1]
    if flip:
        col = ring(value, "dy", y, True)
        own = ring(col.reshape(-1, wide), "dx", x, False)
        own = own.reshape(4, 4, 64, wide).transpose(1, 0, 2, 3).reshape(-1, wide)
    else:
        row = ring(value, "dx", x, True)
        own = ring(row.reshape(-1, wide), "dy", y, False).reshape(-1, wide)
    return own, across(own)


def mm(a, b):
    return jnp.dot(a, b, preferred_element_type=F32)


def mmt(a, b):
    return lax.dot_general(a, b, (((1,), (1,)), ((), ())), preferred_element_type=F32)


def taps_over(values, taps):
    length = values.shape[0]
    padded = jnp.pad(values, ((2, 0), (0, 0)))
    return sum(taps[k] * padded[k : k + length] for k in range(3))


def local(
    tokens,
    mix_gain,
    out_gate_w,
    in_gate_w,
    value_w,
    out_gate_scale,
    in_gate_scale,
    value_scale,
    mix_taps,
    conv_gain,
    out_proj_w,
    proj_scale,
    ffn_gain,
    gate_w,
    up_w,
    gate_scale,
    up_scale,
    gate_taps,
    up_taps,
    gate_bias,
    up_bias,
    down_w,
    down_scale,
):
    fs = lax.axis_index("fs")
    tp = lax.axis_index("tp")
    z, y, x = at = fs // 16, (fs // 4) % 4, fs % 4
    d = mix_gain.shape[0]
    rows = gate_w.shape[0]
    conv, ff = out_gate_w.shape[1], gate_w.shape[1]
    mine = tokens[0]
    half = mine.shape[0]

    gain = lax.dynamic_slice_in_dim(mix_gain, fs * rows, rows)[:, None]
    fgain = lax.dynamic_slice_in_dim(ffn_gain, fs * rows, rows)[:, None]
    first_mix = jnp.concatenate([out_gate_w * gain, in_gate_w * gain], 1).astype(BF16)
    proj = (out_proj_w * conv_gain[:, None] * proj_scale[None]).T
    second_mix = jnp.concatenate([value_w * gain, proj], 1).astype(BF16)
    gate_send = (gate_w * fgain).astype(BF16)
    up_send = (up_w * fgain).astype(BF16)
    down_send = (down_w * down_scale[None]).T.astype(BF16)

    theirs = swap(mine)
    both = placed((mine, theirs), (tp, 1 - tp)).reshape(2 * half, d)
    w1 = zxy(first_mix, at, False)
    w2 = zxy(second_mix, at, True)
    gate_own, gate_oth = xyz(gate_send, at, False)
    up_own, up_oth = xyz(up_send, at, True)
    down_own, down_oth = xyz(down_send, at, False)

    scales = jnp.concatenate([out_gate_scale, in_gate_scale, value_scale, gate_scale, up_scale])
    scales = jnp.pad(scales, (0, 256 - scales.shape[0])).reshape(2, 128)
    scales = lax.all_to_all(
        jnp.broadcast_to(scales[None], (32, 2, 128)), "fs", 0, 0, tiled=True
    ).reshape(32, 256)
    c, f = out_gate_scale.shape[0], gate_scale.shape[0]
    og_s, ig_s, v_s = (scales[:, k * c : (k + 1) * c].reshape(-1) for k in range(3))
    g_s, u_s = (scales[:, 3 * c + k * f : 3 * c + (k + 1) * f].reshape(-1) for k in range(2))
    m_taps = mix_taps * (og_s * ig_s * v_s)
    g_taps = gate_taps * g_s
    u_taps = up_taps * u_s

    wide = both.astype(F32)
    rs = lax.rsqrt(jnp.mean(wide * wide, axis=1, keepdims=True) + EPS)
    acc1 = mm(both, w1)
    acc2 = mm(both, w2[:, :conv])
    inner = acc1[:, conv:] * acc2 * (rs * rs)
    conv_out = acc1[:, :conv] * rs * taps_over(inner, m_taps)
    sumsq = jnp.sum(conv_out * conv_out, axis=1, keepdims=True)
    conv_out = conv_out.astype(BF16)
    proj_w = w2[:, conv:]

    def cut(v, who):
        return lax.dynamic_slice_in_dim(v, who * half, half, 0)

    got_sq = swap(cut(sumsq, 1 - tp))
    got = swap(mmt(cut(conv_out, 1 - tp), proj_w).astype(BF16))
    kept = mmt(cut(conv_out, tp), proj_w)
    rs_c = lax.rsqrt((cut(sumsq, tp) + got_sq) / (2 * conv) + EPS)
    first = (mine.astype(F32) + rs_c * (kept + got.astype(F32))).astype(BF16)

    first_all = placed((first, swap(first)), (tp, 1 - tp)).reshape(2 * half, d)
    wide2 = first_all.astype(F32)
    rs2 = lax.rsqrt(jnp.mean(wide2 * wide2, axis=1, keepdims=True) + EPS)
    x_own = lax.dynamic_slice_in_dim(first_all, z * (d // 2), d // 2, 1)
    x_oth = lax.dynamic_slice_in_dim(first_all, (1 - z) * (d // 2), d // 2, 1)
    gate = (mm(x_own, gate_own) + mm(x_oth, gate_oth)) * rs2
    up = (mm(x_own, up_own) + mm(x_oth, up_oth)) * rs2
    gate_act = taps_over(gate, g_taps) + gate_bias
    up_act = taps_over(up, u_taps) + up_bias
    hidden = lax.optimization_barrier((jax.nn.silu(gate_act) * up_act).astype(BF16))

    h_theirs, h_mine = cut(hidden, 1 - tp), cut(hidden, tp)
    result = jnp.zeros((half, d), BF16)
    for weight, side in ((down_own, z), (down_oth, 1 - z)):
        got = swap(mmt(h_theirs, weight).astype(BF16))
        total = mmt(h_mine, weight) + got.astype(F32)
        start = side * (d // 2)
        base = lax.dynamic_slice_in_dim(first, start, d // 2, 1)
        part = (base.astype(F32) + total).astype(BF16)
        result = lax.dynamic_update_slice_in_dim(result, part, start, 1)
    return result[None]


def solution(mesh):
    specs = (
        P(("rep", "fs"), "tp", None),
        P(),
        P("fs", "tp"),
        P("fs", "tp"),
        P("fs", "tp"),
        P(("tp", "fs")),
        P(("tp", "fs")),
        P(("tp", "fs")),
        P(None, "tp"),
        P("tp"),
        P("tp", "fs"),
        P("fs"),
        P(),
        P("fs", "tp"),
        P("fs", "tp"),
        P(("tp", "fs")),
        P(("tp", "fs")),
        P(None, "tp"),
        P(None, "tp"),
        P("tp"),
        P("tp"),
        P("tp", "fs"),
        P("fs"),
    )
    return jax.shard_map(
        local, mesh=mesh, in_specs=specs, out_specs=P(("rep", "fs"), "tp", None), check_vma=False
    )
```

```python
import jax
import jax.numpy as jnp
from jax import lax
from jax.experimental import pallas as pl
from jax.experimental.pallas import tpu as pltpu
from jax.sharding import PartitionSpec as P


EPS = 1e-06
F32 = jnp.float32
BF16 = jnp.bfloat16
N = 4
BLOCK = 64


def hop(value, a=0, b=0, z=0):
    pairs = []
    for pz in range(N):
        for py in range(N):
            for px in range(N):
                for core in range(2):
                    dx, dy = (b, a) if core else (a, b)
                    to = ((pz + z) % N) * 16 + ((py + dy) % N) * 4 + (px + dx) % N
                    pairs.append(((pz * 16 + py * 4 + px) * 2 + core, to * 2 + core))
    return lax.ppermute(value, ("rep", "fs", "tp"), pairs)


def swap(value):
    return lax.ppermute(value, "tp", [(0, 1), (1, 0)])


def halves(value):
    half = value.shape[0] // 2
    return value[:half], value[half:]


def ring(value, way):
    prev = hop(value, **{way: 1})
    next_ = hop(value, **{way: -1})
    far = (hop(halves(prev)[0], **{way: 1}), hop(halves(next_)[1], **{way: -1}))
    return value, next_, far, prev


def fetch(pieces, spots_ref, refs, weight, sems, groups):
    batches = []
    for g, (at, width) in enumerate(groups):
        batch = []
        for (labels, ref) in zip(pieces, refs):
            for j, t in enumerate(labels):
                to = pl.multiple_of(spots_ref[t] * BLOCK, BLOCK)
                copy = pltpu.make_async_copy(
                    ref.at[pl.ds(BLOCK * j, BLOCK), pl.ds(at, width)],
                    weight.at[pl.ds(to, BLOCK), pl.ds(at, width)],
                    sems.at[g, t],
                )
                copy.start()
                batch.append(copy)
        batches.append(batch)
    return batches


def finish(batch):
    for copy in batch:
        copy.wait()


def call(body, out_shape, pieces, small, weight, n_groups, extra=(), flops=0):
    spec = pl.BlockSpec(memory_space=pltpu.VMEM)
    return pl.pallas_call(
        body,
        out_shape=out_shape,
        in_specs=[pl.BlockSpec(memory_space=pltpu.SMEM)]
        + [pl.BlockSpec(memory_space=pl.ANY)] * len(pieces)
        + [spec] * len(small),
        out_specs=jax.tree.map(lambda _: spec, out_shape),
        scratch_shapes=[
            pltpu.VMEM(weight, BF16),
            pltpu.SemaphoreType.DMA((n_groups, 32)),
            *extra,
        ],
        compiler_params=pltpu.CompilerParams(vmem_limit_bytes=48 * 2**20),
        cost_estimate=pl.CostEstimate(flops=flops, bytes_accessed=2 * weight[0] * weight[1], transcendentals=0),
    )


def shifted(value, last, k):
    if last is None:
        last = jnp.zeros((8, value.shape[1]), value.dtype)
    joined = jnp.concatenate([last[-8:], value], 0)
    return joined[8 - k : 8 - k + value.shape[0]]


ROWS = 256


def mixer(pieces, spots, x, rs, taps):
    arrays = [p for p, _ in pieces]
    labels = [t for _, t in pieces]
    length, depth = x.shape
    wide = arrays[0].shape[1]
    tiles = wide // 384
    groups = ((0, 384), (384, wide - 384))

    def body(spots_ref, *refs):
        ins = refs[: len(arrays)]
        x_ref, rs_ref, taps_ref, out_ref, sq_ref, w_ref, sems = refs[len(arrays) :]
        batches = fetch(labels, spots_ref, ins, w_ref, sems, groups)
        finish(batches[0])
        sq_ref[...] = jnp.zeros_like(sq_ref)

        def tile(n, _):
            @pl.when(n == 1)
            def _():
                finish(batches[1])

            w = w_ref[:, pl.ds(pl.multiple_of(n * 384, 384), 384)]
            at = pl.ds(pl.multiple_of(n * 128, 128), 128)
            tap = taps_ref[:, at]
            last = None
            for m in range(0, length, ROWS):
                acc = jnp.dot(x_ref[m : m + ROWS, :], w, preferred_element_type=F32)
                scale = rs_ref[m : m + ROWS, :]
                inner = acc[:, 128:256] * acc[:, 256:] * (scale * scale)
                total = tap[2:3] * inner
                total += tap[1:2] * shifted(inner, last, 1)
                total += tap[0:1] * shifted(inner, last, 2)
                last = inner
                conv = acc[:, :128] * scale * total
                out_ref[m : m + ROWS, at] = conv.astype(BF16)
                sq_ref[m : m + ROWS, :] += jnp.sum(conv * conv, axis=1, keepdims=True)
            return 0

        lax.fori_loop(0, tiles, tile, 0)

    out = (
        jax.ShapeDtypeStruct((length, wide // 3), BF16),
        jax.ShapeDtypeStruct((length, 1), F32),
    )
    small = (x, rs, taps)
    return call(body, out, arrays, small, (depth, wide), 2, flops=2 * length * depth * wide)(
        spots, *arrays, *small
    )


def gated(pieces, spots, x, rs, g_taps, u_taps, biases):
    arrays = [p for p, _ in pieces]
    labels = [t for _, t in pieces]
    length, depth = x.shape
    wide = arrays[0].shape[1]
    tiles = wide // 256
    groups = ((0, 512), (512, wide - 512))

    def body(spots_ref, *refs):
        ins = refs[: len(arrays)]
        x_ref, rs_ref, g_ref, u_ref, b_ref, out_ref, w_ref, sems = refs[len(arrays) :]
        batches = fetch(labels, spots_ref, ins, w_ref, sems, groups)
        finish(batches[0])

        def tile(n, _):
            @pl.when(n == 2)
            def _():
                finish(batches[1])

            w = w_ref[:, pl.ds(pl.multiple_of(n * 256, 256), 256)]
            at = pl.ds(pl.multiple_of(n * 128, 128), 128)
            tap = jnp.concatenate([g_ref[:, at], u_ref[:, at]], 1)
            bias = jnp.concatenate([b_ref[0:1, at], b_ref[1:2, at]], 1)
            last = None
            for m in range(0, length, ROWS):
                acc = jnp.dot(x_ref[m : m + ROWS, :], w, preferred_element_type=F32)
                acc = acc * rs_ref[m : m + ROWS, :]
                total = bias + tap[2:3] * acc
                total += tap[1:2] * shifted(acc, last, 1)
                total += tap[0:1] * shifted(acc, last, 2)
                last = acc
                gate = total[:, :128]
                out_ref[m : m + ROWS, at] = (gate / (1 + jnp.exp(-gate)) * total[:, 128:]).astype(BF16)
            return 0

        lax.fori_loop(0, tiles, tile, 0)

    out = jax.ShapeDtypeStruct((length, wide // 2), BF16)
    small = (x, rs, g_taps, u_taps, biases)
    return call(body, out, arrays, small, (depth, wide), 2, flops=2 * length * depth * wide)(
        spots, *arrays, *small
    )


def outward(pieces, spots, x, dtype):
    arrays = [p for p, _ in pieces]
    labels = [t for _, t in pieces]
    rows, depth = x.shape
    cols = 32 * BLOCK
    part = 512

    def body(spots_ref, *refs):
        ins = refs[: len(arrays)]
        x_ref, out_ref, w_ref, sems = refs[len(arrays) :]
        (batch,) = fetch(labels, spots_ref, ins, w_ref, sems, ((0, depth),))
        finish(batch)

        def step(n, _):
            at = pl.ds(pl.multiple_of(n * part, part), part)
            out_ref[:, at] = mmt(x_ref[...], w_ref[at, :]).astype(dtype)
            return 0

        lax.fori_loop(0, cols // part, step, 0)

    out = jax.ShapeDtypeStruct((rows, cols), dtype)
    return call(body, out, arrays, (x,), (cols, depth), 1, flops=2 * rows * depth * cols)(
        spots, *arrays, x
    )


def in_turn(arrays):
    depth, wide = arrays[0].shape
    parts = [a.reshape(depth, wide // 128, 1, 128) for a in arrays]
    return jnp.concatenate(parts, 2).reshape(depth, -1)


def mixed(pieces, spots, rows):
    out = jnp.zeros((2, *pieces[0].shape), pieces[0].dtype)
    for piece, spot in zip(pieces, spots):
        out = lax.dynamic_update_index_in_dim(out, piece, spot, 0)
    return out.reshape(rows, pieces[0].shape[1])


def mmt(a, b):
    return lax.dot_general(a, b, (((1,), (1,)), ((), ())), preferred_element_type=F32)


def layer(
    tokens,
    mix_gain,
    out_gate_w,
    in_gate_w,
    value_w,
    out_gate_scale,
    in_gate_scale,
    value_scale,
    mix_taps,
    conv_gain,
    out_proj_w,
    proj_scale,
    ffn_gain,
    gate_w,
    up_w,
    gate_scale,
    up_scale,
    gate_taps,
    up_taps,
    gate_bias,
    up_bias,
    down_w,
    down_scale,
):
    fs = lax.axis_index("fs")
    tp = lax.axis_index("tp")
    z, y, x = fs // 16, (fs // 4) % 4, fs % 4
    rows = gate_w.shape[0]
    conv, ff = out_gate_w.shape[1], gate_w.shape[1]
    mine = tokens[0]
    half = mine.shape[0]

    gain = lax.dynamic_slice_in_dim(mix_gain, fs * rows, rows)[:, None]
    fgain = lax.dynamic_slice_in_dim(ffn_gain, fs * rows, rows)[:, None]
    proj = (out_proj_w * conv_gain[:, None] * proj_scale[None]).T
    mix_send = in_turn([out_gate_w * gain, in_gate_w * gain, value_w * gain])
    mix_send = jnp.concatenate([mix_send, proj], 1).astype(BF16)
    ffn_send = in_turn([gate_w * fgain, up_w * fgain])
    ffn_send = jnp.concatenate([ffn_send, (down_w * down_scale[None]).T], 1)
    ffn_send = ffn_send.astype(BF16)

    theirs = swap(mine)
    both = mixed((mine, theirs), (tp, 1 - tp), 2 * half)

    t = jnp.arange(32, dtype=jnp.int32)
    rz, rb, ra = t // 16, (t // 4) % 4, t % 4
    pa, pb = jnp.where(tp == 0, x, y), jnp.where(tp == 0, y, x)
    ia, ib = (pa + ra) % 4, (pb + rb) % 4
    spots = ((z + rz) % 2) * 16 + jnp.where(tp == 0, ib * 4 + ia, ia * 4 + ib)

    def label(rz, rb, ra):
        return rz * 16 + rb * 4 + ra

    prev, next_ = hop(mix_send, a=1), hop(mix_send, a=-1)
    far = hop(mix_send, a=2)
    line = jnp.concatenate([mix_send, next_, far, prev], 0)
    own, next_, far, prev = ring(line, "b")
    lower = jnp.concatenate([own, next_], 0)
    upper = jnp.concatenate([*far, prev], 0)
    cut_at = 3 * conv
    labels = [[label(rz, rb, ra) for rb in bs for ra in range(4)] for rz in (0, 1) for bs in ((0, 1), (2, 3))]

    def crossed(lo, hi):
        pieces = (lo, hi, hop(lo, z=1), hop(hi, z=-1))
        return list(zip(pieces, labels))

    mix_in = crossed(lower[:, :cut_at], upper[:, :cut_at])
    mix_out = crossed(lower[:, cut_at:], upper[:, cut_at:])

    top, low = halves(ffn_send)
    pair = jnp.concatenate([ffn_send, hop(top, z=1), hop(low, z=-1)], 0)
    own, next_, far, prev = ring(pair, "a")
    line = jnp.concatenate([own, next_, *far, prev], 0)

    def gathered(line):
        own, next_, far, prev = ring(line, "b")
        pieces = [
            (p, [label(rz, rb, ra) for ra in range(4) for rz in (0, 1)])
            for rb, p in ((0, own), (1, next_), (3, prev))
        ]
        pieces += [
            (p, [label(rz, 2, ra) for ra in two for rz in (0, 1)])
            for p, two in zip(far, ((0, 1), (2, 3)))
        ]
        return pieces

    ffn_in = gathered(line[:, : 2 * ff])
    ffn_out = gathered(line[:, 2 * ff :])

    scales = jnp.concatenate([out_gate_scale, in_gate_scale, value_scale, gate_scale, up_scale])
    scales = jnp.pad(scales, (0, 256 - scales.shape[0])).reshape(2, 128)
    scales = lax.all_to_all(
        jnp.broadcast_to(scales[None], (32, 2, 128)), "fs", 0, 0, tiled=True
    ).reshape(32, 256)
    c, f = out_gate_scale.shape[0], gate_scale.shape[0]
    og_s, ig_s, v_s = (scales[:, k * c : (k + 1) * c].reshape(-1) for k in range(3))
    g_s, u_s = (scales[:, 3 * c + k * f : 3 * c + (k + 1) * f].reshape(-1) for k in range(2))
    m_taps = mix_taps * (og_s * ig_s * v_s)
    g_taps = gate_taps * g_s
    u_taps = up_taps * u_s

    wide = both.astype(F32)
    rs = lax.rsqrt(jnp.mean(wide * wide, axis=1, keepdims=True) + EPS)
    conv_out, sumsq = mixer(mix_in, spots, both, rs, m_taps)

    def cut(v, who):
        return lax.dynamic_slice_in_dim(v, who * half, half, 0)

    got_sq = swap(cut(sumsq, 1 - tp))
    got = swap(outward(mix_out, spots, cut(conv_out, 1 - tp), BF16))
    kept = outward(mix_out, spots, cut(conv_out, tp), F32)
    rs_c = lax.rsqrt((cut(sumsq, tp) + got_sq) / (2 * conv) + EPS)
    first = (mine.astype(F32) + rs_c * (kept + got.astype(F32))).astype(BF16)

    first_all = mixed((first, swap(first)), (tp, 1 - tp), 2 * half)
    wide2 = first_all.astype(F32)
    rs2 = lax.rsqrt(jnp.mean(wide2 * wide2, axis=1, keepdims=True) + EPS)
    hidden = gated(
        ffn_in, spots, first_all, rs2, g_taps, u_taps, jnp.stack([gate_bias, up_bias])
    )

    got = swap(outward(ffn_out, spots, cut(hidden, 1 - tp), BF16))
    total = outward(ffn_out, spots, cut(hidden, tp), F32) + got.astype(F32)
    result = (first.astype(F32) + total).astype(BF16)
    return result[None]


def solution(mesh):
    specs = (
        P(("rep", "fs"), "tp", None),
        P(),
        P("fs", "tp"),
        P("fs", "tp"),
        P("fs", "tp"),
        P(("tp", "fs")),
        P(("tp", "fs")),
        P(("tp", "fs")),
        P(None, "tp"),
        P("tp"),
        P("tp", "fs"),
        P("fs"),
        P(),
        P("fs", "tp"),
        P("fs", "tp"),
        P(("tp", "fs")),
        P(("tp", "fs")),
        P(None, "tp"),
        P(None, "tp"),
        P("tp"),
        P("tp"),
        P("tp", "fs"),
        P("fs"),
    )
    return jax.shard_map(
        layer, mesh=mesh, in_specs=specs, out_specs=P(("rep", "fs"), "tp", None), check_vma=False
    )
```

```python
import jax
import jax.numpy as jnp
from jax import lax
from jax.experimental import pallas as pl
from jax.experimental.pallas import tpu as pltpu
from jax.sharding import PartitionSpec as P


EPS = 1e-06
F32 = jnp.float32
BF16 = jnp.bfloat16
N = 4
BLOCK = 64


def hop(value, a=0, b=0, z=0):
    pairs = []
    for pz in range(N):
        for py in range(N):
            for px in range(N):
                for core in range(2):
                    dx, dy = (b, a) if core else (a, b)
                    to = ((pz + z) % N) * 16 + ((py + dy) % N) * 4 + (px + dx) % N
                    pairs.append(((pz * 16 + py * 4 + px) * 2 + core, to * 2 + core))
    return lax.ppermute(value, ("rep", "fs", "tp"), pairs)


def swap(value):
    return lax.ppermute(value, "tp", [(0, 1), (1, 0)])


def halves(value):
    half = value.shape[0] // 2
    return value[:half], value[half:]


def ring(value, way, direct=True):
    prev = hop(value, **{way: 1})
    next_ = hop(value, **{way: -1})
    if direct:
        return value, next_, hop(value, **{way: 2}), prev
    far = (hop(halves(prev)[0], **{way: 1}), hop(halves(next_)[1], **{way: -1}))
    return value, next_, far, prev


def fetch(labels, refs, store, sems, groups):
    batches = []
    for g, (at, width) in enumerate(groups):
        batch, row = [], 0
        for k, (own, ref) in enumerate(zip(labels, refs)):
            size = BLOCK * len(own)
            copy = pltpu.make_async_copy(
                ref.at[:, pl.ds(at, width)],
                store.at[pl.ds(row, size), pl.ds(at, width)],
                sems.at[g, k],
            )
            copy.start()
            batch.append(copy)
            row += size
        batches.append(batch)
    return batches


def arrange(labels, store, spots_ref, put, cols):
    order = [t for own in labels for t in own]
    for k, t in enumerate(order):
        to = pl.ds(pl.multiple_of(spots_ref[t] * BLOCK, BLOCK), BLOCK)
        put(to, store[BLOCK * k : BLOCK * (k + 1), cols])


def finish(batch):
    for copy in batch:
        copy.wait()


def call(body, out_shape, arrays, small, scratch, limit, flops):
    spec = pl.BlockSpec(memory_space=pltpu.VMEM)
    return pl.pallas_call(
        body,
        out_shape=out_shape,
        in_specs=[pl.BlockSpec(memory_space=pltpu.SMEM)]
        + [pl.BlockSpec(memory_space=pltpu.HBM)] * len(arrays)
        + [spec] * len(small),
        out_specs=jax.tree.map(lambda _: spec, out_shape),
        scratch_shapes=scratch,
        compiler_params=pltpu.CompilerParams(vmem_limit_bytes=limit * 2**20),
        cost_estimate=pl.CostEstimate(flops=flops, bytes_accessed=2**23, transcendentals=0),
    )


def row_scale(sides, rs_ref, step=128):
    for s, x_ref in enumerate(sides):
        rows, depth = x_ref.shape
        for m in range(0, rows, step):
            v = x_ref[m : m + step, :].astype(F32)
            mean = jnp.sum(v * v, axis=1, keepdims=True) * (1 / depth)
            rs_ref[s, m : m + step, :] = lax.rsqrt(mean + EPS)


CHUNKS = 4


def staggered(tiles, begin, dot, rest, between):
    def both(n, k, ahead=True, behind=True):
        if ahead:
            begin(n, k)
        for c in range(CHUNKS):
            if ahead:
                dot(n, k, c)
            if behind:
                rest(n - 1, 1 - k, c)

    both(0, 0, behind=False)
    between(0)

    def pair(i, _):
        both(2 * i + 1, 1)

        @pl.when(i == 0)
        def _():
            between(1)

        both(2 * i + 2, 0)
        return 0

    lax.fori_loop(0, (tiles - 1) // 2, pair, 0)
    if tiles % 2 == 0:
        both(tiles - 1, 1)
    both(tiles, tiles % 2, ahead=False)


STEP = 128


def convolved(buf, tap, m, cols):
    total = tap[2:3] * buf[8 + m : 8 + m + STEP, cols]
    total += tap[1:2] * buf[7 + m : 7 + m + STEP, cols]
    return total + tap[0:1] * buf[6 + m : 6 + m + STEP, cols]


def slot_of(m, half, tp):
    return (1 - tp if m < half else tp), m % half


def shared(mine, wide, tile, columns):
    half, depth = mine.shape
    return [
        pltpu.VMEM((2, half, 1), F32),
        pltpu.VMEM((2 * half + 8, columns), F32),
        pltpu.VMEM((2 * half + 8, columns), F32),
        pltpu.VMEM((depth, wide), BF16),
        pltpu.VMEM((depth, tile), BF16),
        pltpu.VMEM((depth, tile), BF16),
        pltpu.SemaphoreType.DMA((3, 5)),
    ]


def product(sides, rs_ref, w, tp, c):
    half = sides[0].shape[0]
    rows = 2 * half // CHUNKS
    s, m = divmod(c * rows, half)
    acc = jnp.dot(sides[s][m : m + rows, :], w[...], preferred_element_type=F32)
    part = (1 - tp, tp)[s]
    at = pl.ds(pl.multiple_of(part * half + m, rows) + 8, rows)
    return at, acc, rs_ref[s, m : m + rows, :]


def mixer(pieces, spots, mine, theirs, taps):
    arrays = [p for p, _ in pieces]
    labels = [t for _, t in pieces]
    half, depth = mine.shape
    length, wide = 2 * half, arrays[0].shape[1]
    groups = ((0, 384), (384, 384), (768, wide - 768))

    def body(spots_ref, *refs):
        ins = refs[: len(arrays)]
        mine_ref, theirs_ref, taps_ref, out_ref, sq_ref, rs_ref, buf_a, buf_b, store, w_a, w_b, sems = (
            refs[len(arrays) :]
        )
        tp = spots_ref[32]
        bufs, weights = (buf_a, buf_b), (w_a, w_b)
        sides = (theirs_ref, mine_ref)
        batches = fetch(labels, ins, store, sems, groups)
        for buf in bufs:
            buf[0:8, :] = jnp.zeros((8, 256), F32)
        row_scale(sides, rs_ref)
        finish(batches[0])

        def begin(n, k):
            def put(to, block):
                weights[k][to, :] = block

            cols = pl.ds(pl.multiple_of(n * 384, 384), 384)
            arrange(labels, store, spots_ref, put, cols)

        def dot(n, k, c):
            at, acc, scale = product(sides, rs_ref, weights[k], tp, c)
            bufs[k][at, 0:128] = acc[:, :128] * scale
            bufs[k][at, 128:] = acc[:, 128:256] * acc[:, 256:] * (scale * scale)

        def rest(n, k, c):
            at = pl.ds(pl.multiple_of(n * 128, 128), 128)
            tap = taps_ref[:, at]
            quarter = length // CHUNKS
            for m in range(c * quarter, (c + 1) * quarter, STEP):
                conv = bufs[k][8 + m : 8 + m + STEP, 0:128]
                conv *= convolved(bufs[k], tap, m, slice(128, 256))
                slot, row = slot_of(m, half, tp)
                out_ref[slot, row : row + STEP, at] = conv.astype(BF16)
                square = jnp.sum(conv * conv, axis=1, keepdims=True)
                first = jnp.zeros_like(square)
                old = sq_ref[slot, row : row + STEP, :]
                sq_ref[slot, row : row + STEP, :] = jnp.where(n == 0, first, old) + square

        staggered(wide // 384, begin, dot, rest, lambda k: finish(batches[k + 1]))

    out = (
        jax.ShapeDtypeStruct((2, half, wide // 3), BF16),
        jax.ShapeDtypeStruct((2, half, 1), F32),
    )
    scratch = shared(mine, wide, 384, 256)
    return call(body, out, arrays, (mine, theirs, taps), scratch, 26, 2 * length * depth * wide)(
        spots, *arrays, mine, theirs, taps
    )


def gated(pieces, spots, mine, theirs, g_taps, u_taps, biases):
    arrays = [p for p, _ in pieces]
    labels = [t for _, t in pieces]
    half, depth = mine.shape
    length, wide = 2 * half, arrays[0].shape[1]
    groups = ((0, 256), (256, 512), (768, wide - 768))

    def body(spots_ref, *refs):
        ins = refs[: len(arrays)]
        mine_ref, theirs_ref, g_ref, u_ref, b_ref, out_ref, rs_ref, buf_a, buf_b, store, w_a, w_b, sems = (
            refs[len(arrays) :]
        )
        tp = spots_ref[32]
        bufs, weights = (buf_a, buf_b), (w_a, w_b)
        sides = (theirs_ref, mine_ref)
        batches = fetch(labels, ins, store, sems, groups)
        for buf in bufs:
            buf[0:8, :] = jnp.zeros((8, 256), F32)
        row_scale(sides, rs_ref)
        finish(batches[0])

        def begin(n, k):
            def put(to, block):
                weights[k][to, :] = block

            cols = pl.ds(pl.multiple_of(n * 256, 256), 256)
            arrange(labels, store, spots_ref, put, cols)

        def dot(n, k, c):
            at, acc, scale = product(sides, rs_ref, weights[k], tp, c)
            bufs[k][at, :] = acc * scale

        def rest(n, k, c):
            at = pl.ds(pl.multiple_of(n * 128, 128), 128)
            tap = jnp.concatenate([g_ref[:, at], u_ref[:, at]], 1)
            bias = jnp.concatenate([b_ref[0:1, at], b_ref[1:2, at]], 1)
            quarter = length // CHUNKS
            for m in range(c * quarter, (c + 1) * quarter, STEP):
                total = bias + convolved(bufs[k], tap, m, slice(0, 256))
                gate = total[:, :128]
                slot, row = slot_of(m, half, tp)
                out_ref[slot, row : row + STEP, at] = (
                    gate / (1 + jnp.exp(-gate)) * total[:, 128:]
                ).astype(BF16)

        staggered(wide // 256, begin, dot, rest, lambda k: finish(batches[k + 1]))

    out = jax.ShapeDtypeStruct((2, half, wide // 2), BF16)
    small = (mine, theirs, g_taps, u_taps, biases)
    scratch = shared(mine, wide, 256, 256)
    return call(body, out, arrays, small, scratch, 32, 2 * length * depth * wide)(
        spots, *arrays, *small
    )


def joined(pieces, spots):
    arrays = [p for p, _ in pieces]
    labels = [t for _, t in pieces]
    beside = len(labels[0][0])
    wide = arrays[0].shape[1] // beside

    def body(spots_ref, *refs):
        out_ref, store, sems = refs[len(arrays) :]
        (batch,) = fetch(labels, refs[: len(arrays)], store, sems, ((0, wide * beside),))
        finish(batch)
        for k in range(beside):

            def put(to, block):
                out_ref[to, :] = block

            one = [[t[k] for t in own] for own in labels]
            arrange(one, store, spots_ref, put, slice(k * wide, (k + 1) * wide))

    out = jax.ShapeDtypeStruct((32 * BLOCK, wide), BF16)
    rows = sum(p.shape[0] for p in arrays)
    scratch = [pltpu.VMEM((rows, wide * beside), BF16), pltpu.SemaphoreType.DMA((1, 5))]
    return call(body, out, arrays, (), scratch, 16, 10**9)(spots, *arrays)


def in_turn(arrays):
    depth, wide = arrays[0].shape
    parts = [a.reshape(depth, wide // 128, 1, 128) for a in arrays]
    return jnp.concatenate(parts, 2).reshape(depth, -1)


def mmt(a, b):
    return lax.dot_general(a, b, (((1,), (1,)), ((), ())), preferred_element_type=F32)


def layer(
    tokens,
    mix_gain,
    out_gate_w,
    in_gate_w,
    value_w,
    out_gate_scale,
    in_gate_scale,
    value_scale,
    mix_taps,
    conv_gain,
    out_proj_w,
    proj_scale,
    ffn_gain,
    gate_w,
    up_w,
    gate_scale,
    up_scale,
    gate_taps,
    up_taps,
    gate_bias,
    up_bias,
    down_w,
    down_scale,
):
    fs = lax.axis_index("fs")
    tp = lax.axis_index("tp")
    z, y, x = fs // 16, (fs // 4) % 4, fs % 4
    rows = gate_w.shape[0]
    conv, ff = out_gate_w.shape[1], gate_w.shape[1]
    mine = tokens[0]

    gain = lax.dynamic_slice_in_dim(mix_gain, fs * rows, rows)[:, None]
    fgain = lax.dynamic_slice_in_dim(ffn_gain, fs * rows, rows)[:, None]
    proj = (out_proj_w * conv_gain[:, None] * proj_scale[None]).T
    mix_send = in_turn([out_gate_w * gain, in_gate_w * gain, value_w * gain])
    mix_send = jnp.concatenate([mix_send, proj], 1).astype(BF16)
    ffn_send = in_turn([gate_w * fgain, up_w * fgain])
    ffn_send = jnp.concatenate([ffn_send, (down_w * down_scale[None]).T], 1)
    ffn_send = ffn_send.astype(BF16)

    theirs = swap(mine)

    t = jnp.arange(32, dtype=jnp.int32)
    rz, rb, ra = t // 16, (t // 4) % 4, t % 4
    pa, pb = jnp.where(tp == 0, x, y), jnp.where(tp == 0, y, x)
    ia, ib = (pa + ra) % 4, (pb + rb) % 4
    spots = ((z + rz) % 2) * 16 + jnp.where(tp == 0, ib * 4 + ia, ia * 4 + ib)
    spots = jnp.concatenate([spots, jnp.full((8,), tp, jnp.int32)])

    def label(rz, rb, ra):
        return rz * 16 + rb * 4 + ra

    line = jnp.concatenate(ring(mix_send, "a"), 0)
    own, next_, far, prev = ring(line, "b")
    cut_at = 3 * conv

    def stack(parts, cols):
        return jnp.concatenate([p[:, cols] for p in parts], 0)

    labels = [[label(rz, rb, ra) for rb in bs for ra in range(4)] for rz in (0, 1) for bs in ((0, 1), (2, 3))]

    def crossed(cols):
        lo, hi = stack((own, next_), cols), stack((far, prev), cols)
        pieces = (lo, hi, hop(lo, z=1), hop(hi, z=-1))
        return list(zip(pieces, labels))

    mix_in = crossed(slice(0, cut_at))
    mix_out = crossed(slice(cut_at, None))

    top, low = halves(ffn_send)
    came = jnp.concatenate([hop(top, z=1), hop(low, z=-1)], 0)
    cut_at = 2 * ff
    down_pair = jnp.concatenate([ffn_send[:, cut_at:], came[:, cut_at:]], 1)
    pair = jnp.concatenate([ffn_send[:, :cut_at], came[:, :cut_at], down_pair], 0)
    line = ring(pair, "a")
    own, next_, far, prev = ring(jnp.concatenate([p[: 2 * BLOCK] for p in line], 0), "b", False)
    ffn_in = [
        (p, [label(rz, rb, ra) for ra in range(4) for rz in (0, 1)])
        for rb, p in ((0, own), (1, next_), (3, prev))
    ]
    ffn_in += [
        (p, [label(rz, 2, ra) for ra in two for rz in (0, 1)])
        for p, two in zip(far, ((0, 1), (2, 3)))
    ]
    down = ring(jnp.concatenate([p[2 * BLOCK :] for p in line], 0), "b")
    ffn_out = [
        (p, [[label(rz, rb, ra) for rz in (0, 1)] for ra in range(4)])
        for rb, p in enumerate(down)
    ]

    scales = jnp.concatenate([out_gate_scale, in_gate_scale, value_scale, gate_scale, up_scale])
    scales = jnp.pad(scales, (0, 256 - scales.shape[0])).reshape(2, 128)
    scales = lax.all_to_all(
        jnp.broadcast_to(scales[None], (32, 2, 128)), "fs", 0, 0, tiled=True
    ).reshape(32, 256)
    c, f = out_gate_scale.shape[0], gate_scale.shape[0]
    og_s, ig_s, v_s = (scales[:, k * c : (k + 1) * c].reshape(-1) for k in range(3))
    g_s, u_s = (scales[:, 3 * c + k * f : 3 * c + (k + 1) * f].reshape(-1) for k in range(2))
    m_taps = mix_taps * (og_s * ig_s * v_s)
    g_taps = gate_taps * g_s
    u_taps = up_taps * u_s

    conv_out, sumsq = mixer(mix_in, spots, mine, theirs, m_taps)
    w_proj = joined([(p, [[t] for t in own]) for p, own in mix_out], spots)
    got_sq = swap(sumsq[0])
    got = swap(mmt(conv_out[0], w_proj).astype(BF16))
    rs_c = lax.rsqrt((sumsq[1] + got_sq) / (2 * conv) + EPS)
    kept = lax.optimization_barrier(mmt(conv_out[1], w_proj).astype(BF16))
    first = kept.astype(F32) + got.astype(F32)
    first = (mine.astype(F32) + rs_c * first).astype(BF16)

    first_theirs = swap(first)
    hidden = gated(
        ffn_in, spots, first, first_theirs, g_taps, u_taps, jnp.stack([gate_bias, up_bias])
    )
    w_down = joined(ffn_out, spots)
    got = swap(mmt(hidden[0], w_down).astype(BF16))
    kept = lax.optimization_barrier(mmt(hidden[1], w_down).astype(BF16))
    total = kept.astype(F32) + got.astype(F32)
    result = (first.astype(F32) + total).astype(BF16)
    return result[None]


def solution(mesh):
    specs = (
        P(("rep", "fs"), "tp", None),
        P(),
        P("fs", "tp"),
        P("fs", "tp"),
        P("fs", "tp"),
        P(("tp", "fs")),
        P(("tp", "fs")),
        P(("tp", "fs")),
        P(None, "tp"),
        P("tp"),
        P("tp", "fs"),
        P("fs"),
        P(),
        P("fs", "tp"),
        P("fs", "tp"),
        P(("tp", "fs")),
        P(("tp", "fs")),
        P(None, "tp"),
        P(None, "tp"),
        P("tp"),
        P("tp"),
        P("tp", "fs"),
        P("fs"),
    )
    return jax.shard_map(layer, mesh=mesh, in_specs=specs, out_specs=P(("rep", "fs"), "tp", None), check_vma=False)
```

```python
import jax
import jax.numpy as jnp
from jax import lax
from jax.experimental import pallas as pl
from jax.experimental.pallas import tpu as pltpu
from jax.sharding import PartitionSpec as P


EPS = 1e-06
F32 = jnp.float32
BF16 = jnp.bfloat16
N = 4
BLOCK = 64


def hop(value, a=0, b=0, z=0):
    pairs = []
    for pz in range(N):
        for py in range(N):
            for px in range(N):
                for core in range(2):
                    dx, dy = (b, a) if core else (a, b)
                    to = ((pz + z) % N) * 16 + ((py + dy) % N) * 4 + (px + dx) % N
                    pairs.append(((pz * 16 + py * 4 + px) * 2 + core, to * 2 + core))
    return lax.ppermute(value, ("rep", "fs", "tp"), pairs)


def swap(value):
    return lax.ppermute(value, "tp", [(0, 1), (1, 0)])


def halves(value):
    half = value.shape[0] // 2
    return value[:half], value[half:]


def ring(value, way, direct=True):
    prev = hop(value, **{way: 1})
    next_ = hop(value, **{way: -1})
    if direct:
        return value, next_, hop(value, **{way: 2}), prev
    far = (hop(halves(prev)[0], **{way: 1}), hop(halves(next_)[1], **{way: -1}))
    return value, next_, far, prev


def fetch(labels, refs, store, sems, groups):
    batches = []
    for g, (at, width) in enumerate(groups):
        batch, row = [], 0
        for k, (own, ref) in enumerate(zip(labels, refs)):
            size = BLOCK * len(own)
            copy = pltpu.make_async_copy(
                ref.at[:, pl.ds(at, width)],
                store.at[pl.ds(row, size), pl.ds(at, width)],
                sems.at[g, k],
            )
            copy.start()
            batch.append(copy)
            row += size
        batches.append(batch)
    return batches


def arrange(labels, store, spots_ref, put, cols):
    order = [t for own in labels for t in own]
    for k, t in enumerate(order):
        to = pl.ds(pl.multiple_of(spots_ref[t] * BLOCK, BLOCK), BLOCK)
        put(to, store[BLOCK * k : BLOCK * (k + 1), cols])


def finish(batch):
    for copy in batch:
        copy.wait()


def call(body, out_shape, arrays, small, scratch, limit, flops):
    spec = pl.BlockSpec(memory_space=pltpu.VMEM)
    return pl.pallas_call(
        body,
        out_shape=out_shape,
        in_specs=[pl.BlockSpec(memory_space=pltpu.SMEM)]
        + [pl.BlockSpec(memory_space=pltpu.HBM)] * len(arrays)
        + [spec] * len(small),
        out_specs=jax.tree.map(lambda _: spec, out_shape),
        scratch_shapes=scratch,
        compiler_params=pltpu.CompilerParams(vmem_limit_bytes=limit * 2**20),
        cost_estimate=pl.CostEstimate(flops=flops, bytes_accessed=2**23, transcendentals=0),
    )


def row_scale(sides, rs_ref, step=128):
    for s, x_ref in enumerate(sides):
        rows, depth = x_ref.shape
        for m in range(0, rows, step):
            v = x_ref[m : m + step, :].astype(F32)
            mean = jnp.sum(v * v, axis=1, keepdims=True) * (1 / depth)
            rs_ref[s, m : m + step, :] = lax.rsqrt(mean + EPS)


CHUNKS = 4


def stacked(parts):
    sizes = [p.shape[0] for p in parts]

    def body(*refs):
        row = 0
        for ref, size in zip(refs, sizes):
            refs[-1][row : row + size, :] = ref[...]
            row += size

    spec = pl.BlockSpec(memory_space=pltpu.VMEM)
    out = jax.ShapeDtypeStruct((sum(sizes), parts[0].shape[1]), BF16)
    return pl.pallas_call(
        body,
        out_shape=out,
        in_specs=[spec] * len(parts),
        out_specs=spec,
        compiler_params=pltpu.CompilerParams(vmem_limit_bytes=10 * 2**20),
        name="stacked",
    )(*parts)


def looped(tiles, begin, dot, rest, between):
    def tile(n, _):
        @pl.when(n == 1)
        def _():
            between()

        begin(n)
        for c in range(CHUNKS):
            dot(n, c)
        for c in range(CHUNKS):
            rest(n, c)
        return 0

    lax.fori_loop(0, tiles, tile, 0)


STEP = 128


def convolved(buf, tap, m, cols):
    total = tap[2:3] * buf[8 + m : 8 + m + STEP, cols]
    total += tap[1:2] * buf[7 + m : 7 + m + STEP, cols]
    return total + tap[0:1] * buf[6 + m : 6 + m + STEP, cols]


def slot_of(m, half, tp):
    return (1 - tp if m < half else tp), m % half


def shared(mine, wide, tile, columns):
    half, depth = mine.shape
    return [
        pltpu.VMEM((2, half, 1), F32),
        pltpu.VMEM((2 * half + 8, columns), F32),
        pltpu.VMEM((depth, wide), BF16),
        pltpu.VMEM((depth, tile), BF16),
        pltpu.SemaphoreType.DMA((2, 8)),
    ]


def product(sides, rs_ref, w, tp, c):
    half = sides[0].shape[0]
    rows = 2 * half // CHUNKS
    s, m = divmod(c * rows, half)
    acc = jnp.dot(sides[s][m : m + rows, :], w[...], preferred_element_type=F32)
    part = (1 - tp, tp)[s]
    at = pl.ds(pl.multiple_of(part * half + m, rows) + 8, rows)
    return at, acc, rs_ref[s, m : m + rows, :]


def mixer(pieces, spots, mine, theirs, taps, wide):
    arrays = [p for p, _ in pieces]
    labels = [t for _, t in pieces]
    half, depth = mine.shape
    length = 2 * half
    groups = ((0, 384), (384, wide - 384))

    def body(spots_ref, *refs):
        ins = refs[: len(arrays)]
        mine_ref, theirs_ref, taps_ref, out_ref, sq_ref, rs_ref, buf, store, w_ref, sems = (
            refs[len(arrays) :]
        )
        tp = spots_ref[32]
        sides = (theirs_ref, mine_ref)
        batches = fetch(labels, ins, store, sems, groups)
        buf[0:8, :] = jnp.zeros((8, 256), F32)
        row_scale(sides, rs_ref)
        finish(batches[0])

        def begin(n):
            def put(to, block):
                w_ref[to, :] = block

            cols = pl.ds(pl.multiple_of(n * 384, 384), 384)
            arrange(labels, store, spots_ref, put, cols)

        def dot(n, c):
            at, acc, scale = product(sides, rs_ref, w_ref, tp, c)
            buf[at, 0:128] = acc[:, :128] * scale
            buf[at, 128:] = acc[:, 128:256] * acc[:, 256:] * (scale * scale)

        def rest(n, c):
            at = pl.ds(pl.multiple_of(n * 128, 128), 128)
            tap = taps_ref[:, at]
            quarter = length // CHUNKS
            for m in range(c * quarter, (c + 1) * quarter, STEP):
                conv = buf[8 + m : 8 + m + STEP, 0:128]
                conv *= convolved(buf, tap, m, slice(128, 256))
                slot, row = slot_of(m, half, tp)
                out_ref[slot, row : row + STEP, at] = conv.astype(BF16)
                square = jnp.sum(conv * conv, axis=1, keepdims=True)
                first = jnp.zeros_like(square)
                old = sq_ref[slot, row : row + STEP, :]
                sq_ref[slot, row : row + STEP, :] = jnp.where(n == 0, first, old) + square

        looped(wide // 384, begin, dot, rest, lambda: finish(batches[1]))

    out = (
        jax.ShapeDtypeStruct((2, half, wide // 3), BF16),
        jax.ShapeDtypeStruct((2, half, 1), F32),
    )
    scratch = shared(mine, wide, 384, 256)
    return call(body, out, arrays, (mine, theirs, taps), scratch, 26, 2 * length * depth * wide)(
        spots, *arrays, mine, theirs, taps
    )


def gated(pieces, spots, mine, theirs, g_taps, u_taps, biases):
    arrays = [p for p, _ in pieces]
    labels = [t for _, t in pieces]
    half, depth = mine.shape
    length, wide = 2 * half, arrays[0].shape[1]
    groups = ((0, 256), (256, wide - 256))

    def body(spots_ref, *refs):
        ins = refs[: len(arrays)]
        mine_ref, theirs_ref, g_ref, u_ref, b_ref, out_ref, rs_ref, buf, store, w_ref, sems = (
            refs[len(arrays) :]
        )
        tp = spots_ref[32]
        sides = (theirs_ref, mine_ref)
        batches = fetch(labels, ins, store, sems, groups)
        buf[0:8, :] = jnp.zeros((8, 256), F32)
        row_scale(sides, rs_ref)
        finish(batches[0])

        def begin(n):
            def put(to, block):
                w_ref[to, :] = block

            cols = pl.ds(pl.multiple_of(n * 256, 256), 256)
            arrange(labels, store, spots_ref, put, cols)

        def dot(n, c):
            at, acc, scale = product(sides, rs_ref, w_ref, tp, c)
            buf[at, :] = acc * scale

        def rest(n, c):
            at = pl.ds(pl.multiple_of(n * 128, 128), 128)
            tap = jnp.concatenate([g_ref[:, at], u_ref[:, at]], 1)
            bias = jnp.concatenate([b_ref[0:1, at], b_ref[1:2, at]], 1)
            quarter = length // CHUNKS
            for m in range(c * quarter, (c + 1) * quarter, STEP):
                total = bias + convolved(buf, tap, m, slice(0, 256))
                gate = total[:, :128]
                slot, row = slot_of(m, half, tp)
                out_ref[slot, row : row + STEP, at] = (
                    gate / (1 + jnp.exp(-gate)) * total[:, 128:]
                ).astype(BF16)

        looped(wide // 256, begin, dot, rest, lambda: finish(batches[1]))

    out = jax.ShapeDtypeStruct((2, half, wide // 2), BF16)
    small = (mine, theirs, g_taps, u_taps, biases)
    scratch = shared(mine, wide, 256, 256)
    return call(body, out, arrays, small, scratch, 32, 2 * length * depth * wide)(
        spots, *arrays, *small
    )


def joined(pieces, spots, start):
    arrays = [p for p, _ in pieces]
    labels = [t for _, t in pieces]
    wide = arrays[0].shape[1] - start

    def body(spots_ref, *refs):
        out_ref, store, sems = refs[len(arrays) :]

        def put(to, block):
            out_ref[to, :] = block

        copies = []
        row = 0
        for k, ref in enumerate(refs[: len(arrays)]):
            rows = arrays[k].shape[0]
            copies.append(
                pltpu.make_async_copy(
                    ref.at[:, pl.ds(start, wide)], store.at[pl.ds(row, rows), :], sems.at[k]
                )
            )
            copies[-1].start()
            row += rows
        finish(copies)
        arrange(labels, store, spots_ref, put, slice(None))

    out = jax.ShapeDtypeStruct((32 * BLOCK, wide), BF16)
    scratch = [pltpu.VMEM(out.shape, BF16), pltpu.SemaphoreType.DMA((8,))]
    return call(body, out, arrays, (), scratch, 16, 10**9)(spots, *arrays)


def in_turn(arrays):
    depth, wide = arrays[0].shape
    parts = [a.reshape(depth, wide // 128, 1, 128) for a in arrays]
    return jnp.concatenate(parts, 2).reshape(depth, -1)


def mmt(a, b):
    return lax.dot_general(a, b, (((1,), (1,)), ((), ())), preferred_element_type=F32)


def layer(
    tokens,
    mix_gain,
    out_gate_w,
    in_gate_w,
    value_w,
    out_gate_scale,
    in_gate_scale,
    value_scale,
    mix_taps,
    conv_gain,
    out_proj_w,
    proj_scale,
    ffn_gain,
    gate_w,
    up_w,
    gate_scale,
    up_scale,
    gate_taps,
    up_taps,
    gate_bias,
    up_bias,
    down_w,
    down_scale,
):
    fs = lax.axis_index("fs")
    tp = lax.axis_index("tp")
    z, y, x = fs // 16, (fs // 4) % 4, fs % 4
    rows = gate_w.shape[0]
    conv = out_gate_w.shape[1]
    mine = tokens[0]

    gain = lax.dynamic_slice_in_dim(mix_gain, fs * rows, rows)[:, None]
    fgain = lax.dynamic_slice_in_dim(ffn_gain, fs * rows, rows)[:, None]
    proj = (out_proj_w * conv_gain[:, None] * proj_scale[None]).T
    mix_send = in_turn([out_gate_w * gain, in_gate_w * gain, value_w * gain])
    mix_send = jnp.concatenate([mix_send, proj], 1).astype(BF16)
    ffn_send = in_turn([gate_w * fgain, up_w * fgain]).astype(BF16)
    down_send = (down_w * down_scale[None]).T.astype(BF16)

    theirs = swap(mine)

    t = jnp.arange(32, dtype=jnp.int32)
    rz, rb, ra = t // 16, (t // 4) % 4, t % 4
    pa, pb = jnp.where(tp == 0, x, y), jnp.where(tp == 0, y, x)
    ia, ib = (pa + ra) % 4, (pb + rb) % 4
    spots = ((z + rz) % 2) * 16 + jnp.where(tp == 0, ib * 4 + ia, ia * 4 + ib)
    spots = jnp.concatenate([spots, jnp.full((8,), tp, jnp.int32)])

    def label(rz, rb, ra):
        return rz * 16 + rb * 4 + ra

    line = stacked(ring(ffn_send, "a"))
    own, next_, far, prev = ring(line, "b", False)
    plane = (own, next_, stacked(far), prev)
    other = [hop(p, z=way) for p, way in zip(plane, (1, 1, -1, -1))]
    ffn_in = [
        (p, [label(rz, rb, ra) for ra in range(4)])
        for rz, side in enumerate((plane, other))
        for rb, p in enumerate(side)
    ]

    send = jnp.concatenate([mix_send, down_send], 1)
    top, low = halves(send)
    came = jnp.concatenate([hop(top, z=1), hop(low, z=-1)], 0)
    cut_at = mix_send.shape[1]

    def paired(mine, cols, direct):
        pair = jnp.concatenate([mine, came[:, cols]], 0)
        line = stacked(ring(pair, "a"))
        own, next_, far, prev = ring(line, "b", direct)
        pieces = [(0, own, range(4)), (1, next_, range(4)), (3, prev, range(4))]
        if direct:
            pieces.append((2, far, range(4)))
        else:
            pieces += [(2, p, two) for p, two in zip(far, ((0, 1), (2, 3)))]
        return [(p, [label(rz, rb, ra) for ra in ras for rz in (0, 1)]) for rb, p, ras in pieces]

    mix_in = paired(mix_send, slice(0, cut_at), False)
    ffn_out = paired(down_send, slice(cut_at, None), True)

    scales = jnp.concatenate([out_gate_scale, in_gate_scale, value_scale, gate_scale, up_scale])
    scales = jnp.pad(scales, (0, 256 - scales.shape[0])).reshape(2, 128)
    scales = lax.all_to_all(
        jnp.broadcast_to(scales[None], (32, 2, 128)), "fs", 0, 0, tiled=True
    ).reshape(32, 256)
    c, f = out_gate_scale.shape[0], gate_scale.shape[0]
    og_s, ig_s, v_s = (scales[:, k * c : (k + 1) * c].reshape(-1) for k in range(3))
    g_s, u_s = (scales[:, 3 * c + k * f : 3 * c + (k + 1) * f].reshape(-1) for k in range(2))
    m_taps = mix_taps * (og_s * ig_s * v_s)
    g_taps = gate_taps * g_s
    u_taps = up_taps * u_s

    biases = jnp.stack([gate_bias, up_bias])
    m_taps, g_taps, u_taps, biases = lax.optimization_barrier((m_taps, g_taps, u_taps, biases))

    conv_out, sumsq = mixer(mix_in, spots, mine, theirs, m_taps, 3 * conv)
    w_proj = joined(mix_in, spots, 3 * conv)
    got_sq = swap(sumsq[0])
    got = swap(mmt(conv_out[0], w_proj).astype(BF16))
    rs_c = lax.rsqrt((sumsq[1] + got_sq) / (2 * conv) + EPS)
    kept = lax.optimization_barrier(mmt(conv_out[1], w_proj).astype(BF16))
    first = kept.astype(F32) + got.astype(F32)
    first = (mine.astype(F32) + rs_c * first).astype(BF16)

    first_theirs = swap(first)
    hidden = gated(
        ffn_in, spots, first, first_theirs, g_taps, u_taps, biases
    )
    w_down = joined(ffn_out, spots, 0)
    got = swap(mmt(hidden[0], w_down).astype(BF16))
    kept = lax.optimization_barrier(mmt(hidden[1], w_down).astype(BF16))
    total = kept.astype(F32) + got.astype(F32)
    result = (first.astype(F32) + total).astype(BF16)
    return result[None]


def solution(mesh):
    specs = (
        P(("rep", "fs"), "tp", None),
        P(),
        P("fs", "tp"),
        P("fs", "tp"),
        P("fs", "tp"),
        P(("tp", "fs")),
        P(("tp", "fs")),
        P(("tp", "fs")),
        P(None, "tp"),
        P("tp"),
        P("tp", "fs"),
        P("fs"),
        P(),
        P("fs", "tp"),
        P("fs", "tp"),
        P(("tp", "fs")),
        P(("tp", "fs")),
        P(None, "tp"),
        P(None, "tp"),
        P("tp"),
        P("tp"),
        P("tp", "fs"),
        P("fs"),
    )
    return jax.shard_map(
        layer, mesh=mesh, in_specs=specs, out_specs=P(("rep", "fs"), "tp", None), check_vma=False
    )
```
